32 devices in a mesh: fs: 8 (over z, x), tp: 4 (over y, core).
Axes of the slice: x: 2, y: 2, z: 4, core: 2. Of those that a mesh axis runs over, the one named last changes fastest.
Arguments:
- tokens: bfloat16 [1024, 2048], P('fs'), may hold values from -6 to 6
- gain: float32 [2048], P('fs'), may hold values from 0.1 to 1.9
- up_master: float32 [2048, 8192], P('fs', 'tp'), may hold values from -0.125 to 0.125
- down_master: float32 [2048, 8192], P('fs', 'tp'), may hold values from -0.0625 to 0.0625
Outputs:
- up_sampled: bfloat16 [8, 2048, 1024], P('fs', None, 'tp')
- down_sampled: bfloat16 [8, 2048, 1024], P('fs', None, 'tp')
- mixed: bfloat16 [1024, 2048], P('fs', 'tp')
The draws below stay inside these ranges and needn't reach their ends.
All inputs are finite; a program needn't handle non-finite values.
Results may differ from the reference program's by a relative error of at most 0.0087.
Values may be sent and summed in bfloat16 or wider, within the bound.
A program may use at most 64 MiB of HBM per device.

```python
import jax
import jax.numpy as jnp
from jax import lax

D = 2048
FF = 8192
SUB = 8
TOKENS = 1024
UNITS_DEV = 256
N_FS = 8
N_TP = 4


def levels(stream_key, shape, split, smallest, largest):
    def one(axis_at, shards_of):
        draws = jax.random.uniform(jax.random.fold_in(jax.random.fold_in(stream_key, 6), axis_at), (shards_of,), jnp.float32, smallest / len(split), largest / len(split))
        return jnp.repeat(jnp.exp(draws), shape[axis_at] // shards_of).reshape((-1,) + (1,) * (len(shape) - axis_at - 1))

    level = one(*split[0])
    for cut in split[1:]:
        level = level * one(*cut)
    return level


def centred(stream_key, shape, width, bound, split=(), kind=jnp.bfloat16):
    drawn = width * jax.random.normal(stream_key, shape, jnp.float32)
    if split:
        drawn = drawn * levels(stream_key, shape, split, -0.22, 0.18)
    return jnp.clip(drawn, -bound, bound).astype(kind)


def setup_inputs(seed: int = 0) -> dict:
    key_list = jax.random.split(jax.random.key(seed), 5)
    tokens = centred(key_list[0], (TOKENS, D), 1.0, 6.0, ((0, 8),))
    gain = jnp.clip(1.0 + 0.18 * jax.random.normal(key_list[1], (D,), jnp.float32), 0.1, 1.9)
    up_master = centred(key_list[2], (D, FF), D ** -0.5, 0.125, ((0, 8), (1, 4)), jnp.float32)
    down_master = centred(key_list[3], (D, FF), FF ** -0.5, 0.0625, ((0, 8), (1, 4)), jnp.float32)
    return dict(tokens=tokens, gain=gain, up_master=up_master, down_master=down_master)


def sampled(weight):
    blocks = weight.reshape(D, N_TP, SUB, UNITS_DEV).transpose(2, 0, 1, 3).reshape(SUB, D, N_TP * UNITS_DEV)
    return jnp.tile(blocks, (N_FS // SUB, 1, 1))

def reference(tokens, gain, up_master, down_master):
    up_round = (gain[:, None] * up_master).astype(jnp.bfloat16)
    down_round = down_master.astype(jnp.bfloat16)
    widened = tokens.astype(jnp.float32)
    normed = (widened * lax.rsqrt(lax.optimization_barrier(jnp.mean(widened * widened, axis=1, keepdims=True)) + 1e-06)).astype(jnp.bfloat16)
    pre_units = jnp.dot(normed, up_round, preferred_element_type=jnp.float32)
    act_units = jnp.square(jax.nn.relu(pre_units)).astype(jnp.bfloat16)
    mixed = lax.dot_general(act_units, down_round, (((1,), (1,)), ((), ())), preferred_element_type=jnp.float32)
    return (sampled(up_round), sampled(down_round), mixed.astype(jnp.bfloat16))
```

```python
import functools

import jax
import jax.numpy as jnp
from jax import lax
from jax.experimental import pallas as pl
from jax.experimental.pallas import tpu as pltpu
from jax.sharding import PartitionSpec as P

SUB = 8
EPS = 1e-06
BF16 = jnp.bfloat16
F32 = jnp.float32


def fused(
    nz, tok, gain, upm, dnm, up_o, dn_o, mix_o,
    xg, up_s, dn_s, act, cs, cr, ys, yr, xs, xb, xr, zb, zr,
    s_tz, r_tz, s_tx, r_tx, s_ty, r_ty, s_tc, r_tc,
    s_up, r_up, s_dn, r_dn, s_c, r_c, s_y, r_y, s_x, r_x, s_z, r_z,
):
    f, t = lax.axis_index("fs"), lax.axis_index("tp")
    z, x = f // 2, f % 2
    y, c = t // 2, t % 2
    ox, oy, oc = 1 - x, 1 - y, 1 - c
    rows, width = tok.shape
    cols = width // 4
    feat = upm.shape[0]
    units = act.shape[1]
    at_x = (z * 2 + ox, t)
    at_y = (f, oy * 2 + c)
    at_c = (f, y * 2 + oc)

    barrier = pltpu.get_barrier_semaphore()
    for d in range(1, SUB):
        pl.semaphore_signal(barrier, inc=1, device_id=((f + d) % SUB, t),
                            device_id_type=pl.DeviceIdType.MESH)
    for dev in (at_y, at_c):
        pl.semaphore_signal(barrier, inc=1, device_id=dev, device_id_type=pl.DeviceIdType.MESH)

    sent = []

    def send(src, dst, ssem, rsem, dev):
        copy = pltpu.make_async_remote_copy(
            src_ref=src, dst_ref=dst, send_sem=ssem, recv_sem=rsem,
            device_id=dev, device_id_type=pl.DeviceIdType.MESH)
        copy.start()
        sent.append(copy)

    def arrived(dst, ssem, rsem, dev):
        pltpu.make_async_remote_copy(
            src_ref=dst, dst_ref=dst, send_sem=ssem, recv_sem=rsem,
            device_id=dev, device_id_type=pl.DeviceIdType.MESH).wait_recv()

    low = 1 - z // 2
    far = (3 * low, 1 + low, 1 - z + 4 * (1 - low))

    wide = tok[...].astype(F32)
    scale = lax.rsqrt(jnp.mean(wide * wide, axis=1, keepdims=True) + EPS)
    mine = tok[:, pl.ds(pl.multiple_of(t * cols, cols), cols)].astype(F32)
    xg[t, z, x] = (mine * scale).astype(BF16)
    pl.semaphore_wait(barrier, SUB + 1)

    for zz in far:
        send(xg.at[t, z, x], xg.at[t, z, x], s_tz.at[zz], r_tz.at[z], (zz * 2 + x, t))

    def pass_on(zz):
        send(xg.at[t, zz, x], xg.at[t, zz, x], s_tx.at[zz], r_tx.at[zz], at_x)
        send(xg.at[t, zz, x], xg.at[t, zz, x], s_ty.at[zz, x], r_ty.at[zz, x], at_y)

    pass_on(z)

    def cast(src, dst, out, factor):
        for m in range(SUB):
            block = src[:, m * units:(m + 1) * units]
            dst[m] = (block if factor is None else factor * block).astype(BF16)
        block = src[:, pl.ds(pl.multiple_of(f * units, units), units)]
        out[pl.ds(pl.multiple_of(f * feat, feat), feat), :] = (
            block if factor is None else factor * block).astype(BF16)

    def at_rows(ref, k):
        return ref.at[pl.ds(pl.multiple_of(k * feat, feat), feat), :]

    def scatter(src, out, ssem, rsem):
        order = [zz * 2 + xx for zz in far for xx in (x, ox)] + [z * 2 + ox]
        for dest in order:
            send(src.at[dest], at_rows(out, f), ssem.at[dest], rsem.at[f], (dest, t))

    cast(upm, up_s, up_o, gain[...])
    scatter(up_s, up_o, s_up, r_up)
    cast(dnm, dn_s, dn_o, None)
    scatter(dn_s, dn_o, s_dn, r_dn)

    near = (far[2], far[1], far[0])
    for zz in near:
        arrived(xg.at[t, zz, x], s_tz.at[zz], r_tz.at[zz], (zz * 2 + x, t))
        pass_on(zz)
    for xx in (x,):
        send(xg.at[t, :, xx], xg.at[t, :, xx], s_tc.at[y, xx], r_tc.at[y, xx], at_c)
    for zz in (z,) + near:
        arrived(xg.at[t, zz, ox], s_tx.at[zz], r_tx.at[zz], at_x)
        send(xg.at[t, zz, ox], xg.at[t, zz, ox], s_ty.at[zz, ox], r_ty.at[zz, ox], at_y)
    send(xg.at[t, :, ox], xg.at[t, :, ox], s_tc.at[y, ox], r_tc.at[y, ox], at_c)
    other = oy * 2 + c
    for xx in (x, ox):
        for zz in (z,) + near:
            arrived(xg.at[other, zz, xx], s_ty.at[zz, xx], r_ty.at[zz, xx], at_y)
        send(xg.at[other, :, xx], xg.at[other, :, xx], s_tc.at[oy, xx], r_tc.at[oy, xx], at_c)
    for yy in (y, oy):
        for xx in (x, ox):
            part = xg.at[yy * 2 + oc, :, xx]
            arrived(part, s_tc.at[yy, xx], r_tc.at[yy, xx], at_c)

    everyone = [zz * 2 + xx for zz in far for xx in (x, ox)] + [z * 2 + ox]
    for k in everyone:
        arrived(at_rows(up_o, k), s_up.at[k], r_up.at[k], (k, t))

    span = 2 * rows

    @pl.loop(0, nz)
    def _(zz):
        total = jnp.zeros((span, units), F32)
        for q in range(4):
            total += jnp.dot(xg[q, zz].reshape(span, cols), up_o[q * cols:(q + 1) * cols, :],
                             preferred_element_type=F32)
        act[pl.ds(pl.multiple_of(zz * span, span), span), :] = jnp.square(
            jnp.maximum(total, 0.0)).astype(BF16)

    def partial(k, zz):
        return lax.dot_general(
            act[pl.ds(pl.multiple_of(zz * span, span), span), :],
            dn_o[pl.ds(pl.multiple_of(k * feat, feat), feat), :],
            (((1,), (1,)), ((), ())), preferred_element_type=F32)

    def have(k):
        @pl.when(k != f)
        def _():
            arrived(at_rows(dn_o, k), s_dn.at[k], r_dn.at[k], (k, t))

    def to_core(yy, i):
        k = yy * 4 + oc * 2 + i
        have(k)

        @pl.loop(0, nz)
        def _(zz):
            cs[yy * 2 + i, zz] = partial(k, zz).astype(BF16)

        send(cs.at[yy * 2 + i], cr.at[yy * 2 + i], s_c.at[yy, i], r_c.at[yy, i], at_c)

    def core_sum(yy, i):
        have(yy * 4 + c * 2 + i)
        arrived(cr.at[yy * 2 + i], s_c.at[yy, i], r_c.at[yy, i], at_c)

    for i in range(2):
        to_core(oy, i)
    for i in range(2):
        core_sum(oy, i)

        @pl.loop(0, nz)
        def _(zz):
            ys[i, zz] = (partial(oy * 4 + c * 2 + i, zz) + cr[oy * 2 + i, zz].astype(F32)).astype(BF16)

        send(ys.at[i], yr.at[i], s_y.at[i], r_y.at[i], at_y)
    for i in range(2):
        to_core(y, i)
    for i in range(2):
        core_sum(y, i)
        arrived(yr.at[i], s_y.at[i], r_y.at[i], at_y)

        @pl.loop(0, nz)
        def _(zz):
            total = (partial(y * 4 + c * 2 + i, zz) + cr[y * 2 + i, zz].astype(F32)
                     + yr[i, zz].astype(F32))
            for xx in range(2):
                half = total[xx * rows:(xx + 1) * rows]
                xs[i, xx, zz] = half
                xb[i, xx, zz] = half.astype(BF16)

        send(xb.at[i, ox], xr.at[i], s_x.at[i], r_x.at[i], at_x)
    for i in range(2):
        arrived(xr.at[i], s_x.at[i], r_x.at[i], at_x)

        @pl.loop(0, nz)
        def _(zz):
            total = xs[i, x, zz] + xr[i, zz].astype(F32)
            xs[i, x, zz] = total
            zb[i, zz] = total.astype(BF16)

        for zz in far:
            send(zb.at[i, zz], zr.at[i, z], s_z.at[i, zz], r_z.at[i, z], (zz * 2 + x, t))
    for i in range(2):
        total = xs[i, x, z]
        for zz in near:
            arrived(zr.at[i, zz], s_z.at[i, zz], r_z.at[i, zz], (zz * 2 + x, t))
            total += zr[i, zz].astype(F32)
        mix_o[:, i * feat:(i + 1) * feat] = total.astype(BF16)
    for copy in sent:
        copy.wait_send()


def on_device_fused(tokens, gain, up_master, down_master):
    rows, width = tokens.shape
    feat, ff = up_master.shape
    units = ff // SUB
    nz = SUB // 2
    cols = width // 4
    span = 2 * rows
    dma = pltpu.SemaphoreType.DMA
    vmem = pl.BlockSpec(memory_space=pltpu.VMEM)
    shapes = [(nz,), (nz,), (nz, 2), (2, 2), (SUB,), (SUB,), (2, 2), (2,), (2,), (2, nz)]
    up_s, dn_s, mixed = pl.pallas_call(
        functools.partial(fused, nz),
        out_shape=(
            jax.ShapeDtypeStruct((SUB * feat, units), BF16),
            jax.ShapeDtypeStruct((SUB * feat, units), BF16),
            jax.ShapeDtypeStruct((rows, cols), BF16),
        ),
        in_specs=[vmem] * 4,
        out_specs=(vmem,) * 3,
        scratch_shapes=[
            pltpu.VMEM((4, nz, 2, rows, cols), BF16),
            pltpu.VMEM((SUB, feat, units), BF16),
            pltpu.VMEM((SUB, feat, units), BF16),
            pltpu.VMEM((SUB * rows, units), BF16),
            pltpu.VMEM((4, nz, span, feat), BF16),
            pltpu.VMEM((4, nz, span, feat), BF16),
            pltpu.VMEM((2, nz, span, feat), BF16),
            pltpu.VMEM((2, nz, span, feat), BF16),
            pltpu.VMEM((2, 2, nz, rows, feat), F32),
            pltpu.VMEM((2, 2, nz, rows, feat), BF16),
            pltpu.VMEM((2, nz, rows, feat), BF16),
            pltpu.VMEM((2, nz, rows, feat), BF16),
            pltpu.VMEM((2, nz, rows, feat), BF16),
        ] + [dma(shape) for shape in shapes for _ in range(2)],
        compiler_params=pltpu.CompilerParams(
            collective_id=0, has_side_effects=True, vmem_limit_bytes=60 * 2**20),
    )(tokens, gain[:, None], up_master, down_master)
    return up_s[None], dn_s[None], mixed


def from_partner(block, axis, bit):
    count = lax.axis_size(axis)
    route = []
    for low in range(count):
        high = low | 1 << bit
        if high != low and high < count:
            route += [(low, high), (high, low)]
    return lax.ppermute(block, axis, route)


def on_device(tokens, gain, up_master, down_master):
    fs_count = lax.axis_size("fs")
    feat_rows = up_master.shape[0]
    units = up_master.shape[1] // SUB
    groups_count = fs_count // SUB
    member = lax.axis_index("fs") % SUB
    up_round = (gain[:, None] * up_master).astype(jnp.bfloat16)
    down_round = down_master.astype(jnp.bfloat16)

    def spread(weight):
        blocks = weight.reshape(feat_rows, SUB, units).transpose(1, 0, 2)
        return jnp.broadcast_to(blocks[None], (groups_count, SUB, feat_rows, units)).reshape(
            fs_count, feat_rows, units
        )

    up_sampled, down_sampled = (
        lax.all_to_all(spread(up_round), "fs", split_axis=0, concat_axis=1, tiled=True),
        lax.all_to_all(spread(down_round), "fs", split_axis=0, concat_axis=1, tiled=True),
    )
    levels = SUB.bit_length() - 1
    bit_list = list(range(levels))
    widened = tokens.astype(jnp.float32)
    normed = (
        widened * lax.rsqrt(jnp.mean(widened * widened, axis=1, keepdims=True) + 1e-06)
    ).astype(jnp.bfloat16)
    current = normed[None]
    for bit in bit_list:
        partner = from_partner(current, "fs", bit)
        lower = member >> bit & 1 == 0
        current = jnp.where(lower, jnp.stack([current, partner]), jnp.stack([partner, current]))
    order_now = list(reversed(bit_list))
    wanted = list(range(levels - 1, -1, -1))
    perm_axes = [
        [place for place, value in enumerate(order_now) if value == target][0] for target in wanted
    ]
    current = jnp.transpose(current, perm_axes + [levels, levels + 1, levels + 2])
    gathered = current.reshape(SUB * tokens.shape[0], tokens.shape[1])
    pre_units = jnp.dot(gathered, up_sampled[0], preferred_element_type=jnp.float32)
    act_units = jnp.square(jax.nn.relu(pre_units)).astype(jnp.bfloat16)
    partial_out = lax.dot_general(
        act_units, down_sampled[0], (((1,), (1,)), ((), ())), preferred_element_type=jnp.float32
    )
    running = partial_out.reshape((2,) * levels + (tokens.shape[0], tokens.shape[1]))
    axis_bits = list(range(levels - 1, -1, -1))
    for bit in bit_list:
        position = len([value for value in axis_bits if value > bit])
        mine = member >> bit & 1
        keep = lax.dynamic_index_in_dim(running, mine, position, keepdims=False)
        other = lax.dynamic_index_in_dim(running, 1 - mine, position, keepdims=False)
        running = keep + from_partner(other, "fs", bit)
        axis_bits = [value for value in axis_bits if value != bit]
    summed = lax.psum_scatter(running, "tp", scatter_dimension=1, tiled=True)
    return (up_sampled, down_sampled, summed.astype(jnp.bfloat16))


def solution(mesh):
    placed = (P("fs", None), P("fs"), P("fs", "tp"), P("fs", "tp"))
    one_group = mesh.shape["fs"] == SUB and mesh.shape["tp"] == 4
    return jax.shard_map(
        on_device_fused if one_group else on_device,
        mesh=mesh,
        in_specs=placed,
        out_specs=(P("fs", None, "tp"), P("fs", None, "tp"), P("fs", "tp")),
        check_vma=False,
    )
```

```python
import functools

import jax
import jax.numpy as jnp
from jax import lax
from jax.experimental import pallas as pl
from jax.experimental.pallas import tpu as pltpu
from jax.sharding import PartitionSpec as P

SUB = 8
EPS = 1e-06
BF16 = jnp.bfloat16
F32 = jnp.float32


def fused(
    nz, tok, gain, upm, dnm, up_o, dn_o, mix_o,
    xg, up_s, dn_s, act, cs, cr, fw, fb, yr, gs, gb, gr, hb, hr, xs, xb, xr, kept, zb, zr,
    s_tz, r_tz, s_tx, r_tx, s_ty, r_ty, s_tc, r_tc,
    s_up, r_up, s_dn, r_dn, s_c, r_c, s_y, r_y, s_g, r_g, s_h, r_h, s_x, r_x, s_z, r_z,
):
    f, t = lax.axis_index("fs"), lax.axis_index("tp")
    z, x = f // 2, f % 2
    y, c = t // 2, t % 2
    ox, oy, oc = 1 - x, 1 - y, 1 - c
    rows, width = tok.shape
    cols = width // 4
    feat = upm.shape[0]
    units = act.shape[1]
    at_x = (z * 2 + ox, t)
    at_y = (f, oy * 2 + c)
    at_c = (f, y * 2 + oc)

    barrier = pltpu.get_barrier_semaphore()
    for d in range(1, SUB):
        pl.semaphore_signal(barrier, inc=1, device_id=((f + d) % SUB, t),
                            device_id_type=pl.DeviceIdType.MESH)
    for dev in (at_y, at_c):
        pl.semaphore_signal(barrier, inc=1, device_id=dev, device_id_type=pl.DeviceIdType.MESH)

    sent = []

    def send(src, dst, ssem, rsem, dev):
        copy = pltpu.make_async_remote_copy(
            src_ref=src, dst_ref=dst, send_sem=ssem, recv_sem=rsem,
            device_id=dev, device_id_type=pl.DeviceIdType.MESH)
        copy.start()
        sent.append(copy)

    def arrived(dst, ssem, rsem, dev):
        pltpu.make_async_remote_copy(
            src_ref=dst, dst_ref=dst, send_sem=ssem, recv_sem=rsem,
            device_id=dev, device_id_type=pl.DeviceIdType.MESH).wait_recv()

    low = 1 - z // 2
    far = (3 * low, 1 + low, 1 - z + 4 * (1 - low))

    turn = (far[0] * c + far[2] * (1 - c), far[1], far[2] * c + far[0] * (1 - c))

    wide = tok[...].astype(F32)
    scale = lax.rsqrt(jnp.mean(wide * wide, axis=1, keepdims=True) + EPS)
    mine = tok[:, pl.ds(pl.multiple_of(t * cols, cols), cols)].astype(F32)
    xg[t, z, x] = (mine * scale).astype(BF16)
    pl.semaphore_wait(barrier, SUB + 1)

    for zz in turn:
        send(xg.at[t, z, x], xg.at[t, z, x], s_tz.at[zz], r_tz.at[z], (zz * 2 + x, t))

    def pass_on(zz):
        send(xg.at[t, zz, x], xg.at[t, zz, x], s_tx.at[zz], r_tx.at[zz], at_x)
        send(xg.at[t, zz, x], xg.at[t, zz, x], s_ty.at[zz, x], r_ty.at[zz, x], at_y)

    pass_on(z)

    def cast(src, dst, out, factor):
        for m in range(SUB):
            block = src[:, m * units:(m + 1) * units]
            dst[m] = (block if factor is None else factor * block).astype(BF16)
        block = src[:, pl.ds(pl.multiple_of(f * units, units), units)]
        out[pl.ds(pl.multiple_of(f * feat, feat), feat), :] = (
            block if factor is None else factor * block).astype(BF16)

    def at_rows(ref, k):
        return ref.at[pl.ds(pl.multiple_of(k * feat, feat), feat), :]

    def scatter(src, out, ssem, rsem):
        order = [z * 2 + ox] + [zz * 2 + xx for zz in turn for xx in (x, ox)]
        for dest in order:
            send(src.at[dest], at_rows(out, f), ssem.at[dest], rsem.at[f], (dest, t))

    cast(upm, up_s, up_o, gain[...])
    scatter(up_s, up_o, s_up, r_up)
    cast(dnm, dn_s, dn_o, None)
    scatter(dn_s, dn_o, s_dn, r_dn)

    near = (far[2], far[1], far[0])
    for zz in near:
        arrived(xg.at[t, zz, x], s_tz.at[zz], r_tz.at[zz], (zz * 2 + x, t))
        pass_on(zz)
    for xx in (x,):
        send(xg.at[t, :, xx], xg.at[t, :, xx], s_tc.at[y, xx], r_tc.at[y, xx], at_c)
    for zz in (z,) + near:
        arrived(xg.at[t, zz, ox], s_tx.at[zz], r_tx.at[zz], at_x)
        send(xg.at[t, zz, ox], xg.at[t, zz, ox], s_ty.at[zz, ox], r_ty.at[zz, ox], at_y)
    send(xg.at[t, :, ox], xg.at[t, :, ox], s_tc.at[y, ox], r_tc.at[y, ox], at_c)
    other = oy * 2 + c
    for xx in (x, ox):
        for zz in (z,) + near:
            arrived(xg.at[other, zz, xx], s_ty.at[zz, xx], r_ty.at[zz, xx], at_y)
        send(xg.at[other, :, xx], xg.at[other, :, xx], s_tc.at[oy, xx], r_tc.at[oy, xx], at_c)
    for yy in (y, oy):
        for xx in (x, ox):
            part = xg.at[yy * 2 + oc, :, xx]
            arrived(part, s_tc.at[yy, xx], r_tc.at[yy, xx], at_c)

    everyone = [zz * 2 + xx for zz in far for xx in (x, ox)] + [z * 2 + ox]
    for k in everyone:
        arrived(at_rows(up_o, k), s_up.at[k], r_up.at[k], (k, t))

    span = 2 * rows

    @pl.loop(0, nz)
    def _(zz):
        total = jnp.zeros((span, units), F32)
        for q in range(4):
            total += jnp.dot(xg[q, zz].reshape(span, cols), up_o[q * cols:(q + 1) * cols, :],
                             preferred_element_type=F32)
        act[pl.ds(pl.multiple_of(zz * span, span), span), :] = jnp.square(
            jnp.maximum(total, 0.0)).astype(BF16)

    def partial(k, zz):
        return lax.dot_general(
            act[pl.ds(pl.multiple_of(zz * span, span), span), :],
            dn_o[pl.ds(pl.multiple_of(k * feat, feat), feat), :],
            (((1,), (1,)), ((), ())), preferred_element_type=F32)

    def have(k):
        @pl.when(k != f)
        def _():
            arrived(at_rows(dn_o, k), s_dn.at[k], r_dn.at[k], (k, t))

    def two(h):
        return pl.ds(h * 2, 2)

    def each(h, body):
        @pl.loop(0, 2)
        def _(step):
            body(h * 2 + step)

    def to_core(yy, i):
        k = yy * 4 + oc * 2 + i
        have(k)

        @pl.loop(0, nz)
        def _(zz):
            cs[yy * 2 + i, zz] = partial(k, zz).astype(BF16)

        send(cs.at[yy * 2 + i], cr.at[yy * 2 + i], s_c.at[yy, i], r_c.at[yy, i], at_c)

    def core_sum(yy, i, zz):
        return partial(yy * 4 + c * 2 + i, zz) + cr[yy * 2 + i, zz].astype(F32)

    def halves(total, wide_ref, sent_ref, zz):
        for xx in range(2):
            half = total[xx * rows:(xx + 1) * rows]
            wide_ref[xx, zz] = half
            sent_ref[xx, zz] = half.astype(BF16)

    hs = (low, 1 - low)
    close = z // 2
    over_y = [
        pltpu.make_async_remote_copy(
            src_ref=fb.at[oy, two(h)], dst_ref=yr.at[two(h)], send_sem=s_y.at[h],
            recv_sem=r_y.at[h], device_id=at_y, device_id_type=pl.DeviceIdType.MESH)
        for h in hs]
    sent.extend(over_y)

    for yy in (close, 1 - close):
        for i in (1, 0):
            to_core(yy, i)
        for i in (1, 0):
            have(yy * 4 + c * 2 + i)
            arrived(cr.at[yy * 2 + i], s_c.at[yy, i], r_c.at[yy, i], at_c)
            for h in hs:
                if i == 1:
                    each(h, lambda zz: halves(core_sum(yy, 1, zz), gs.at[yy], gb.at[yy], zz))
                    send(gb.at[yy, ox, two(h)], gr.at[yy, two(h)],
                         s_g.at[yy, h], r_g.at[yy, h], at_x)
                else:
                    def body(zz):
                        total = core_sum(yy, 0, zz)
                        fw[yy, zz] = total
                        fb[yy, zz] = total.astype(BF16)

                    each(h, body)

        @pl.when(yy == oy)
        def _():
            for copy in over_y:
                copy.start()

    for h in hs:
        arrived(gr.at[oy, two(h)], s_g.at[oy, h], r_g.at[oy, h], at_x)

        def body(zz):
            hb[zz] = (gs[oy, x, zz] + gr[oy, zz].astype(F32)).astype(BF16)

        each(h, body)
        send(hb.at[two(h)], hr.at[two(h)], s_h.at[h], r_h.at[h], at_y)
    for h in hs:
        arrived(yr.at[two(h)], s_y.at[h], r_y.at[h], at_y)
        each(h, lambda zz: halves(fw[y, zz] + yr[zz].astype(F32), xs, xb, zz))
        send(xb.at[ox, two(h)], xr.at[two(h)], s_x.at[h], r_x.at[h], at_x)

    def over_z(i, place):
        for zz in (far[:2], far[2:])[place]:
            send(zb.at[i, zz], zr.at[i, z], s_z.at[i, zz], r_z.at[i, z], (zz * 2 + x, t))

    for place, h in enumerate(hs):
        arrived(gr.at[y, two(h)], s_g.at[y, h], r_g.at[y, h], at_x)
        arrived(hr.at[two(h)], s_h.at[h], r_h.at[h], at_y)

        def body(zz):
            total = gs[y, x, zz] + gr[y, zz].astype(F32) + hr[zz].astype(F32)
            kept[1, zz] = total
            zb[1, zz] = total.astype(BF16)

        each(h, body)
        over_z(1, place)
    for place, h in enumerate(hs):
        arrived(xr.at[two(h)], s_x.at[h], r_x.at[h], at_x)

        def body(zz):
            total = xs[x, zz] + xr[zz].astype(F32)
            kept[0, zz] = total
            zb[0, zz] = total.astype(BF16)

        each(h, body)
        over_z(0, place)
    for i in (1, 0):
        total = kept[i, z]
        for zz in near:
            arrived(zr.at[i, zz], s_z.at[i, zz], r_z.at[i, zz], (zz * 2 + x, t))
            total += zr[i, zz].astype(F32)
        mix_o[:, i * feat:(i + 1) * feat] = total.astype(BF16)
    for copy in sent:
        copy.wait_send()


def on_device_fused(tokens, gain, up_master, down_master):
    rows, width = tokens.shape
    feat, ff = up_master.shape
    units = ff // SUB
    nz = SUB // 2
    cols = width // 4
    span = 2 * rows
    dma = pltpu.SemaphoreType.DMA
    vmem = pl.BlockSpec(memory_space=pltpu.VMEM)
    shapes = [(nz,), (nz,), (nz, 2), (2, 2), (SUB,), (SUB,), (2, 2), (2,), (2, 2), (2,), (2,), (2, nz)]
    up_s, dn_s, mixed = pl.pallas_call(
        functools.partial(fused, nz),
        out_shape=(
            jax.ShapeDtypeStruct((SUB * feat, units), BF16),
            jax.ShapeDtypeStruct((SUB * feat, units), BF16),
            jax.ShapeDtypeStruct((rows, cols), BF16),
        ),
        in_specs=[vmem] * 4,
        out_specs=(vmem,) * 3,
        scratch_shapes=[
            pltpu.VMEM((4, nz, 2, rows, cols), BF16),
            pltpu.VMEM((SUB, feat, units), BF16),
            pltpu.VMEM((SUB, feat, units), BF16),
            pltpu.VMEM((SUB * rows, units), BF16),
            pltpu.VMEM((4, nz, span, feat), BF16),
            pltpu.VMEM((4, nz, span, feat), BF16),
            pltpu.VMEM((2, nz, span, feat), F32),
            pltpu.VMEM((2, nz, span, feat), BF16),
            pltpu.VMEM((nz, span, feat), BF16),
            pltpu.VMEM((2, 2, nz, rows, feat), F32),
            pltpu.VMEM((2, 2, nz, rows, feat), BF16),
            pltpu.VMEM((2, nz, rows, feat), BF16),
            pltpu.VMEM((nz, rows, feat), BF16),
            pltpu.VMEM((nz, rows, feat), BF16),
            pltpu.VMEM((2, nz, rows, feat), F32),
            pltpu.VMEM((2, nz, rows, feat), BF16),
            pltpu.VMEM((nz, rows, feat), BF16),
            pltpu.VMEM((2, nz, rows, feat), F32),
            pltpu.VMEM((2, nz, rows, feat), BF16),
            pltpu.VMEM((2, nz, rows, feat), BF16),
        ] + [dma(shape) for shape in shapes for _ in range(2)],
        compiler_params=pltpu.CompilerParams(
            collective_id=0, has_side_effects=True, vmem_limit_bytes=60 * 2**20),
    )(tokens, gain[:, None], up_master, down_master)
    return up_s[None], dn_s[None], mixed


def from_partner(block, axis, bit):
    count = lax.axis_size(axis)
    route = []
    for low in range(count):
        high = low | 1 << bit
        if high != low and high < count:
            route += [(low, high), (high, low)]
    return lax.ppermute(block, axis, route)


def on_device(tokens, gain, up_master, down_master):
    fs_count = lax.axis_size("fs")
    feat_rows = up_master.shape[0]
    units = up_master.shape[1] // SUB
    groups_count = fs_count // SUB
    member = lax.axis_index("fs") % SUB
    up_round = (gain[:, None] * up_master).astype(jnp.bfloat16)
    down_round = down_master.astype(jnp.bfloat16)

    def spread(weight):
        blocks = weight.reshape(feat_rows, SUB, units).transpose(1, 0, 2)
        return jnp.broadcast_to(blocks[None], (groups_count, SUB, feat_rows, units)).reshape(
            fs_count, feat_rows, units
        )

    up_sampled, down_sampled = (
        lax.all_to_all(spread(up_round), "fs", split_axis=0, concat_axis=1, tiled=True),
        lax.all_to_all(spread(down_round), "fs", split_axis=0, concat_axis=1, tiled=True),
    )
    levels = SUB.bit_length() - 1
    bit_list = list(range(levels))
    widened = tokens.astype(jnp.float32)
    normed = (
        widened * lax.rsqrt(jnp.mean(widened * widened, axis=1, keepdims=True) + 1e-06)
    ).astype(jnp.bfloat16)
    current = normed[None]
    for bit in bit_list:
        partner = from_partner(current, "fs", bit)
        lower = member >> bit & 1 == 0
        current = jnp.where(lower, jnp.stack([current, partner]), jnp.stack([partner, current]))
    order_now = list(reversed(bit_list))
    wanted = list(range(levels - 1, -1, -1))
    perm_axes = [
        [place for place, value in enumerate(order_now) if value == target][0] for target in wanted
    ]
    current = jnp.transpose(current, perm_axes + [levels, levels + 1, levels + 2])
    gathered = current.reshape(SUB * tokens.shape[0], tokens.shape[1])
    pre_units = jnp.dot(gathered, up_sampled[0], preferred_element_type=jnp.float32)
    act_units = jnp.square(jax.nn.relu(pre_units)).astype(jnp.bfloat16)
    partial_out = lax.dot_general(
        act_units, down_sampled[0], (((1,), (1,)), ((), ())), preferred_element_type=jnp.float32
    )
    running = partial_out.reshape((2,) * levels + (tokens.shape[0], tokens.shape[1]))
    axis_bits = list(range(levels - 1, -1, -1))
    for bit in bit_list:
        position = len([value for value in axis_bits if value > bit])
        mine = member >> bit & 1
        keep = lax.dynamic_index_in_dim(running, mine, position, keepdims=False)
        other = lax.dynamic_index_in_dim(running, 1 - mine, position, keepdims=False)
        running = keep + from_partner(other, "fs", bit)
        axis_bits = [value for value in axis_bits if value != bit]
    summed = lax.psum_scatter(running, "tp", scatter_dimension=1, tiled=True)
    return (up_sampled, down_sampled, summed.astype(jnp.bfloat16))


def solution(mesh):
    placed = (P("fs", None), P("fs"), P("fs", "tp"), P("fs", "tp"))
    one_group = mesh.shape["fs"] == SUB and mesh.shape["tp"] == 4
    return jax.shard_map(
        on_device_fused if one_group else on_device,
        mesh=mesh,
        in_specs=placed,
        out_specs=(P("fs", None, "tp"), P("fs", None, "tp"), P("fs", "tp")),
        check_vma=False,
    )
```

```python
import functools

import jax
import jax.numpy as jnp
from jax import lax
from jax.experimental import pallas as pl
from jax.experimental.pallas import tpu as pltpu
from jax.sharding import PartitionSpec as P

SUB = 8
EPS = 1e-06
BF16 = jnp.bfloat16
F32 = jnp.float32


def fused(
    nz, tok_h, gain, upm_h, dnm_h, up_h, dn_h, mix_o,
    tok, upm, dnm, up_o, dn_o, s_in, s_out, xg, up_s, dn_s, act, cs, cr, fw, fb, yr, gs, gb, gr, hb, hr, xs, xb, xr, kept, zb, zr,
    s_tz, r_tz, s_tx, r_tx, s_ty, r_ty, s_tc, r_tc,
    s_up, r_up, s_dn, r_dn, s_c, r_c, s_y, r_y, s_g, r_g, s_h, r_h, s_x, r_x, s_z, r_z,
):
    f, t = lax.axis_index("fs"), lax.axis_index("tp")
    z, x = f // 2, f % 2
    y, c = t // 2, t % 2
    ox, oy, oc = 1 - x, 1 - y, 1 - c
    rows, width = tok.shape
    cols = width // 4
    feat = upm.shape[0]
    units = act.shape[1]
    at_x = (z * 2 + ox, t)
    at_y = (f, oy * 2 + c)
    at_c = (f, y * 2 + oc)

    fetch = [pltpu.make_async_copy(src, dst, s_in.at[n]) for n, (src, dst) in enumerate(
        ((tok_h, tok), (upm_h, upm), (dnm_h, dnm)))]
    for copy in fetch:
        copy.start()

    barrier = pltpu.get_barrier_semaphore()
    for d in range(1, SUB):
        pl.semaphore_signal(barrier, inc=1, device_id=((f + d) % SUB, t),
                            device_id_type=pl.DeviceIdType.MESH)
    for dev in (at_y, at_c):
        pl.semaphore_signal(barrier, inc=1, device_id=dev, device_id_type=pl.DeviceIdType.MESH)

    sent = []

    def send(src, dst, ssem, rsem, dev):
        copy = pltpu.make_async_remote_copy(
            src_ref=src, dst_ref=dst, send_sem=ssem, recv_sem=rsem,
            device_id=dev, device_id_type=pl.DeviceIdType.MESH)
        copy.start()
        sent.append(copy)

    def arrived(dst, ssem, rsem, dev):
        pltpu.make_async_remote_copy(
            src_ref=dst, dst_ref=dst, send_sem=ssem, recv_sem=rsem,
            device_id=dev, device_id_type=pl.DeviceIdType.MESH).wait_recv()

    low = 1 - z // 2
    far = (3 * low, 1 + low, 1 - z + 4 * (1 - low))

    turn = (far[0] * c + far[2] * (1 - c), far[1], far[2] * c + far[0] * (1 - c))

    fetch[0].wait()
    wide = tok[...].astype(F32)
    scale = lax.rsqrt(jnp.mean(wide * wide, axis=1, keepdims=True) + EPS)
    mine = tok[:, pl.ds(pl.multiple_of(t * cols, cols), cols)].astype(F32)
    xg[t, z, x] = (mine * scale).astype(BF16)
    pl.semaphore_wait(barrier, SUB + 1)

    for zz in turn:
        send(xg.at[t, z, x], xg.at[t, z, x], s_tz.at[zz], r_tz.at[z], (zz * 2 + x, t))

    def pass_on(zz):
        send(xg.at[t, zz, x], xg.at[t, zz, x], s_tx.at[zz], r_tx.at[zz], at_x)
        send(xg.at[t, zz, x], xg.at[t, zz, x], s_ty.at[zz, x], r_ty.at[zz, x], at_y)

    pass_on(z)

    def cast(src, dst, out, factor):
        for m in range(SUB):
            block = src[:, m * units:(m + 1) * units]
            dst[m] = (block if factor is None else factor * block).astype(BF16)
        block = src[:, pl.ds(pl.multiple_of(f * units, units), units)]
        out[pl.ds(pl.multiple_of(f * feat, feat), feat), :] = (
            block if factor is None else factor * block).astype(BF16)

    def at_rows(ref, k):
        return ref.at[pl.ds(pl.multiple_of(k * feat, feat), feat), :]

    def order(planes):
        return [z * 2 + ox] + [zz * 2 + xx for zz in planes for xx in (x, ox)]

    fine = feat // 2

    def at_half(ref, k, i):
        return ref.at[pl.ds(pl.multiple_of(k * feat + i * fine, fine), fine), :]

    fetch[1].wait()
    cast(upm, up_s, up_o, jnp.transpose(gain[...]))
    for dest in order(turn):
        send(up_s.at[dest], at_rows(up_o, f), s_up.at[dest], r_up.at[f], (dest, t))
    fetch[2].wait()
    cast(dnm, dn_s, dn_o, None)

    near = (far[2], far[1], far[0])
    for zz in near:
        arrived(xg.at[t, zz, x], s_tz.at[zz], r_tz.at[zz], (zz * 2 + x, t))
        pass_on(zz)
    for xx in (x,):
        send(xg.at[t, :, xx], xg.at[t, :, xx], s_tc.at[y, xx], r_tc.at[y, xx], at_c)
    for zz in (z,) + near:
        arrived(xg.at[t, zz, ox], s_tx.at[zz], r_tx.at[zz], at_x)
        send(xg.at[t, zz, ox], xg.at[t, zz, ox], s_ty.at[zz, ox], r_ty.at[zz, ox], at_y)
    send(xg.at[t, :, ox], xg.at[t, :, ox], s_tc.at[y, ox], r_tc.at[y, ox], at_c)
    other = oy * 2 + c
    for xx in (x, ox):
        for zz in (z,) + near:
            arrived(xg.at[other, zz, xx], s_ty.at[zz, xx], r_ty.at[zz, xx], at_y)
        send(xg.at[other, :, xx], xg.at[other, :, xx], s_tc.at[oy, xx], r_tc.at[oy, xx], at_c)
    def send_down(i, dest):
        send(dn_s.at[dest, i * fine:(i + 1) * fine], at_half(dn_o, f, i),
             s_dn.at[i, dest], r_dn.at[i, f], (dest, t))

    for i in range(2):
        for dest in order(far[2:]):
            send_down(i, dest)
    for yy in (y, oy):
        for xx in (x, ox):
            part = xg.at[yy * 2 + oc, :, xx]
            arrived(part, s_tc.at[yy, xx], r_tc.at[yy, xx], at_c)

    everyone = [zz * 2 + xx for zz in far for xx in (x, ox)] + [z * 2 + ox]
    for k in everyone:
        arrived(at_rows(up_o, k), s_up.at[k], r_up.at[k], (k, t))
    crossing = (far[0] * c + far[1] * (1 - c), far[1] * c + far[0] * (1 - c))
    for i in range(2):
        for zz in crossing:
            for xx in (x, ox):
                send_down(i, zz * 2 + xx)
    keep_up = pltpu.make_async_copy(up_o, up_h, s_out.at[0])
    keep_up.start()

    span = 2 * rows

    @pl.loop(0, nz)
    def _(zz):
        total = jnp.zeros((span, units), F32)
        for q in range(4):
            total += jnp.dot(xg[q, zz].reshape(span, cols), up_o[q * cols:(q + 1) * cols, :],
                             preferred_element_type=F32)
        act[pl.ds(pl.multiple_of(zz * span, span), span), :] = jnp.square(
            jnp.maximum(total, 0.0)).astype(BF16)

    def partial(yy, cc, i, zz):
        rows_act = act[pl.ds(pl.multiple_of(zz * span, span), span), :]
        return jnp.concatenate([
            lax.dot_general(
                rows_act, at_half(dn_o, yy * 4 + cc * 2 + xx, i)[...],
                (((1,), (1,)), ((), ())), preferred_element_type=F32)
            for xx in range(2)], axis=1)

    def have(yy, cc, i):
        for xx in range(2):
            k = yy * 4 + cc * 2 + xx

            @pl.when(k != f)
            def _():
                arrived(at_half(dn_o, k, i), s_dn.at[i, k], r_dn.at[i, k], (k, t))

    def two(h):
        return pl.ds(h * 2, 2)

    def each(h, body):
        @pl.loop(0, 2)
        def _(step):
            body(h * 2 + step)

    def to_core(yy, i):
        have(yy, oc, i)

        @pl.loop(0, nz)
        def _(zz):
            cs[yy * 2 + i, zz] = partial(yy, oc, i, zz).astype(BF16)

        send(cs.at[yy * 2 + i], cr.at[yy * 2 + i], s_c.at[yy, i], r_c.at[yy, i], at_c)

    def core_sum(yy, i, zz):
        return partial(yy, c, i, zz) + cr[yy * 2 + i, zz].astype(F32)

    def halves(total, wide_ref, sent_ref, zz):
        for xx in range(2):
            half = total[xx * rows:(xx + 1) * rows]
            wide_ref[xx, zz] = half
            sent_ref[xx, zz] = half.astype(BF16)

    hs = (low, 1 - low)
    close = z // 2
    over_y = [
        pltpu.make_async_remote_copy(
            src_ref=fb.at[oy, two(h)], dst_ref=yr.at[two(h)], send_sem=s_y.at[h],
            recv_sem=r_y.at[h], device_id=at_y, device_id_type=pl.DeviceIdType.MESH)
        for h in hs]
    sent.extend(over_y)

    def stage(i, yy):
        to_core(yy, i)
        have(yy, c, i)
        arrived(cr.at[yy * 2 + i], s_c.at[yy, i], r_c.at[yy, i], at_c)
        for h in hs:
            if i == 1:
                each(h, lambda zz: halves(core_sum(yy, 1, zz), gs.at[yy], gb.at[yy], zz))
                send(gb.at[yy, ox, two(h)], gr.at[yy, two(h)],
                     s_g.at[yy, h], r_g.at[yy, h], at_x)
            else:
                def body(zz):
                    total = core_sum(yy, 0, zz)
                    fw[yy, zz] = total
                    fb[yy, zz] = total.astype(BF16)

                each(h, body)
        if i == 0:
            @pl.when(yy == oy)
            def _():
                for copy in over_y:
                    copy.start()

    pair, same = far[2], (z + 2) % 4
    across = (pair + 2) % 4
    at_pair, at_same = (pair * 2 + x, t), (same * 2 + x, t)

    def to_pair(i, place):
        if place == 0:
            send(zb.at[i, across], zr.at[i, 0], s_z.at[i, 0], r_z.at[i, 0], at_pair)
        else:
            send(zb.at[i, pair], zr.at[i, 1], s_z.at[i, 1], r_z.at[i, 1], at_pair)

    def cross(i):
        arrived(zr.at[i, 0], s_z.at[i, 0], r_z.at[i, 0], at_pair)
        zb[i, z] = (kept[i, same] + zr[i, 0].astype(F32)).astype(BF16)
        send(zb.at[i, z], zr.at[i, 2], s_z.at[i, 2], r_z.at[i, 2], at_same)

    stage(0, close)
    stage(1, close)
    stage(0, 1 - close)
    for h in hs:
        arrived(yr.at[two(h)], s_y.at[h], r_y.at[h], at_y)
        each(h, lambda zz: halves(fw[y, zz] + yr[zz].astype(F32), xs, xb, zz))
        send(xb.at[ox, two(h)], xr.at[two(h)], s_x.at[h], r_x.at[h], at_x)
    stage(1, 1 - close)
    keep_dn = pltpu.make_async_copy(dn_o, dn_h, s_out.at[1])
    keep_dn.start()
    for place, h in enumerate(hs):
        arrived(gr.at[oy, two(h)], s_g.at[oy, h], r_g.at[oy, h], at_x)

        def body(zz):
            hb[zz] = (gs[oy, x, zz] + gr[oy, zz].astype(F32)).astype(BF16)

        each(h, body)
        send(hb.at[two(h)], hr.at[two(h)], s_h.at[h], r_h.at[h], at_y)
    for place, h in enumerate(hs):
        arrived(xr.at[two(h)], s_x.at[h], r_x.at[h], at_x)

        def body(zz):
            total = xs[x, zz] + xr[zz].astype(F32)
            kept[0, zz] = total

            @pl.when(zz != z)
            def _():
                zb[0, zz] = total.astype(BF16)

        each(h, body)
        to_pair(0, place)
    cross(0)
    for place, h in enumerate(hs):
        arrived(gr.at[y, two(h)], s_g.at[y, h], r_g.at[y, h], at_x)
        arrived(hr.at[two(h)], s_h.at[h], r_h.at[h], at_y)

        def body(zz):
            total = gs[y, x, zz] + gr[y, zz].astype(F32) + hr[zz].astype(F32)
            kept[1, zz] = total

            @pl.when(zz != z)
            def _():
                zb[1, zz] = total.astype(BF16)

        each(h, body)
        to_pair(1, place)
        if place == 0:
            cross(1)
    for i in range(2):
        arrived(zr.at[i, 1], s_z.at[i, 1], r_z.at[i, 1], at_pair)
        arrived(zr.at[i, 2], s_z.at[i, 2], r_z.at[i, 2], at_same)
        total = (kept[i, z] + zr[i, 1].astype(F32) + zr[i, 2].astype(F32)).astype(BF16)
        for xx in range(2):
            mix_o[:, xx * feat + i * fine:xx * feat + (i + 1) * fine] = (
                total[:, xx * fine:(xx + 1) * fine])
    for copy in sent:
        copy.wait_send()
    keep_up.wait()
    keep_dn.wait()


def on_device_fused(tokens, gain, up_master, down_master):
    rows, width = tokens.shape
    feat, ff = up_master.shape
    units = ff // SUB
    nz = SUB // 2
    cols = width // 4
    span = 2 * rows
    dma = pltpu.SemaphoreType.DMA
    vmem = pl.BlockSpec(memory_space=pltpu.VMEM)
    anywhere = pl.BlockSpec(memory_space=pl.ANY)
    shapes = [(nz,), (nz,), (nz, 2), (2, 2), (SUB,), (2, SUB), (2, 2), (2,), (2, 2), (2,), (2,), (2, nz)]
    up_s, dn_s, mixed = pl.pallas_call(
        functools.partial(fused, nz),
        out_shape=(
            jax.ShapeDtypeStruct((SUB * feat, units), BF16),
            jax.ShapeDtypeStruct((SUB * feat, units), BF16),
            jax.ShapeDtypeStruct((rows, cols), BF16),
        ),
        in_specs=[anywhere, vmem, anywhere, anywhere],
        out_specs=(anywhere, anywhere, vmem),
        scratch_shapes=[
            pltpu.VMEM((rows, width), BF16),
            pltpu.VMEM((feat, ff), F32),
            pltpu.VMEM((feat, ff), F32),
            pltpu.VMEM((SUB * feat, units), BF16),
            pltpu.VMEM((SUB * feat, units), BF16),
            dma((3,)),
            dma((2,)),
            pltpu.VMEM((4, nz, 2, rows, cols), BF16),
            pltpu.VMEM((SUB, feat, units), BF16),
            pltpu.VMEM((SUB, feat, units), BF16),
            pltpu.VMEM((SUB * rows, units), BF16),
            pltpu.VMEM((4, nz, span, feat), BF16),
            pltpu.VMEM((4, nz, span, feat), BF16),
            pltpu.VMEM((2, nz, span, feat), F32),
            pltpu.VMEM((2, nz, span, feat), BF16),
            pltpu.VMEM((nz, span, feat), BF16),
            pltpu.VMEM((2, 2, nz, rows, feat), F32),
            pltpu.VMEM((2, 2, nz, rows, feat), BF16),
            pltpu.VMEM((2, nz, rows, feat), BF16),
            pltpu.VMEM((nz, rows, feat), BF16),
            pltpu.VMEM((nz, rows, feat), BF16),
            pltpu.VMEM((2, nz, rows, feat), F32),
            pltpu.VMEM((2, nz, rows, feat), BF16),
            pltpu.VMEM((nz, rows, feat), BF16),
            pltpu.VMEM((2, nz, rows, feat), F32),
            pltpu.VMEM((2, nz, rows, feat), BF16),
            pltpu.VMEM((2, nz, rows, feat), BF16),
        ] + [dma(shape) for shape in shapes for _ in range(2)],
        compiler_params=pltpu.CompilerParams(
            collective_id=0, has_side_effects=True, vmem_limit_bytes=60 * 2**20),
    )(tokens, gain[None, :], up_master, down_master)
    return up_s[None], dn_s[None], mixed


def from_partner(block, axis, bit):
    count = lax.axis_size(axis)
    route = []
    for low in range(count):
        high = low | 1 << bit
        if high != low and high < count:
            route += [(low, high), (high, low)]
    return lax.ppermute(block, axis, route)


def on_device(tokens, gain, up_master, down_master):
    fs_count = lax.axis_size("fs")
    feat_rows = up_master.shape[0]
    units = up_master.shape[1] // SUB
    groups_count = fs_count // SUB
    member = lax.axis_index("fs") % SUB
    up_round = (gain[:, None] * up_master).astype(jnp.bfloat16)
    down_round = down_master.astype(jnp.bfloat16)

    def spread(weight):
        blocks = weight.reshape(feat_rows, SUB, units).transpose(1, 0, 2)
        return jnp.broadcast_to(blocks[None], (groups_count, SUB, feat_rows, units)).reshape(
            fs_count, feat_rows, units
        )

    up_sampled, down_sampled = (
        lax.all_to_all(spread(up_round), "fs", split_axis=0, concat_axis=1, tiled=True),
        lax.all_to_all(spread(down_round), "fs", split_axis=0, concat_axis=1, tiled=True),
    )
    levels = SUB.bit_length() - 1
    bit_list = list(range(levels))
    widened = tokens.astype(jnp.float32)
    normed = (
        widened * lax.rsqrt(jnp.mean(widened * widened, axis=1, keepdims=True) + 1e-06)
    ).astype(jnp.bfloat16)
    current = normed[None]
    for bit in bit_list:
        partner = from_partner(current, "fs", bit)
        lower = member >> bit & 1 == 0
        current = jnp.where(lower, jnp.stack([current, partner]), jnp.stack([partner, current]))
    order_now = list(reversed(bit_list))
    wanted = list(range(levels - 1, -1, -1))
    perm_axes = [
        [place for place, value in enumerate(order_now) if value == target][0] for target in wanted
    ]
    current = jnp.transpose(current, perm_axes + [levels, levels + 1, levels + 2])
    gathered = current.reshape(SUB * tokens.shape[0], tokens.shape[1])
    pre_units = jnp.dot(gathered, up_sampled[0], preferred_element_type=jnp.float32)
    act_units = jnp.square(jax.nn.relu(pre_units)).astype(jnp.bfloat16)
    partial_out = lax.dot_general(
        act_units, down_sampled[0], (((1,), (1,)), ((), ())), preferred_element_type=jnp.float32
    )
    running = partial_out.reshape((2,) * levels + (tokens.shape[0], tokens.shape[1]))
    axis_bits = list(range(levels - 1, -1, -1))
    for bit in bit_list:
        position = len([value for value in axis_bits if value > bit])
        mine = member >> bit & 1
        keep = lax.dynamic_index_in_dim(running, mine, position, keepdims=False)
        other = lax.dynamic_index_in_dim(running, 1 - mine, position, keepdims=False)
        running = keep + from_partner(other, "fs", bit)
        axis_bits = [value for value in axis_bits if value != bit]
    summed = lax.psum_scatter(running, "tp", scatter_dimension=1, tiled=True)
    return (up_sampled, down_sampled, summed.astype(jnp.bfloat16))


def solution(mesh):
    placed = (P("fs", None), P("fs"), P("fs", "tp"), P("fs", "tp"))
    one_group = mesh.shape["fs"] == SUB and mesh.shape["tp"] == 4
    return jax.shard_map(
        on_device_fused if one_group else on_device,
        mesh=mesh,
        in_specs=placed,
        out_specs=(P("fs", None, "tp"), P("fs", None, "tp"), P("fs", "tp")),
        check_vma=False,
    )
```

```python
import functools

import jax
import jax.numpy as jnp
from jax import lax
from jax.experimental import pallas as pl
from jax.experimental.pallas import tpu as pltpu
from jax.sharding import PartitionSpec as P

SUB = 8
EPS = 1e-06
BF16 = jnp.bfloat16
F32 = jnp.float32


def fused(
    nz, tok_h, gain, upm_h, dnm_h, up_h, dn_h, mix_o,
    tok, upm, dnm, up_o, dn_o, s_in, s_out, xg, up_s, dn_s, act, cs, cr, fw, fb, yr, gs, gb, gr, hb, hr, xs, xb, xr, kept, zb, zr,
    s_tz, r_tz, s_tx, r_tx, s_ty, r_ty, s_tc, r_tc,
    s_up, r_up, s_dn, r_dn, s_c, r_c, s_y, r_y, s_g, r_g, s_h, r_h, s_x, r_x, s_z, r_z,
):
    f, t = lax.axis_index("fs"), lax.axis_index("tp")
    z, x = f // 2, f % 2
    y, c = t // 2, t % 2
    ox, oy, oc = 1 - x, 1 - y, 1 - c
    rows, width = tok.shape
    cols = width // 4
    feat = upm.shape[0]
    units = act.shape[1]
    at_x = (z * 2 + ox, t)
    at_y = (f, oy * 2 + c)
    at_c = (f, y * 2 + oc)

    fetch = [pltpu.make_async_copy(src, dst, s_in.at[n]) for n, (src, dst) in enumerate(
        ((tok_h, tok), (upm_h, upm), (dnm_h, dnm)))]
    for copy in fetch:
        copy.start()

    barrier = pltpu.get_barrier_semaphore()
    for d in range(1, SUB):
        pl.semaphore_signal(barrier, inc=1, device_id=((f + d) % SUB, t),
                            device_id_type=pl.DeviceIdType.MESH)
    for dev in (at_y, at_c):
        pl.semaphore_signal(barrier, inc=1, device_id=dev, device_id_type=pl.DeviceIdType.MESH)

    sent = []

    def send(src, dst, ssem, rsem, dev):
        copy = pltpu.make_async_remote_copy(
            src_ref=src, dst_ref=dst, send_sem=ssem, recv_sem=rsem,
            device_id=dev, device_id_type=pl.DeviceIdType.MESH)
        copy.start()
        sent.append(copy)

    def arrived(dst, ssem, rsem, dev):
        pltpu.make_async_remote_copy(
            src_ref=dst, dst_ref=dst, send_sem=ssem, recv_sem=rsem,
            device_id=dev, device_id_type=pl.DeviceIdType.MESH).wait_recv()

    low = 1 - z // 2
    far = (3 * low, 1 + low, 1 - z + 4 * (1 - low))

    turn = (far[0] * c + far[2] * (1 - c), far[1], far[2] * c + far[0] * (1 - c))

    fetch[0].wait()
    wide = tok[...].astype(F32)
    scale = lax.rsqrt(jnp.mean(wide * wide, axis=1, keepdims=True) + EPS)
    mine = tok[:, pl.ds(pl.multiple_of(t * cols, cols), cols)].astype(F32)
    xg[t, z, x] = (mine * scale).astype(BF16)
    pl.semaphore_wait(barrier, SUB + 1)

    for zz in turn:
        send(xg.at[t, z, x], xg.at[t, z, x], s_tz.at[zz], r_tz.at[z], (zz * 2 + x, t))

    def pass_on(zz):
        send(xg.at[t, zz, x], xg.at[t, zz, x], s_tx.at[zz], r_tx.at[zz], at_x)
        send(xg.at[t, zz, x], xg.at[t, zz, x], s_ty.at[zz, x], r_ty.at[zz, x], at_y)

    pass_on(z)

    def cast(src, dst, out, factor):
        for m in range(SUB):
            block = src[:, m * units:(m + 1) * units]
            dst[m] = (block if factor is None else factor * block).astype(BF16)
        block = src[:, pl.ds(pl.multiple_of(f * units, units), units)]
        out[pl.ds(pl.multiple_of(f * feat, feat), feat), :] = (
            block if factor is None else factor * block).astype(BF16)

    def at_rows(ref, k):
        return ref.at[pl.ds(pl.multiple_of(k * feat, feat), feat), :]

    def order(planes):
        return [z * 2 + ox] + [zz * 2 + xx for zz in planes for xx in (x, ox)]

    fine = feat // 2

    def at_half(ref, k, i):
        return ref.at[pl.ds(pl.multiple_of(k * feat + i * fine, fine), fine), :]

    fetch[1].wait()
    cast(upm, up_s, up_o, jnp.transpose(gain[...]))
    for dest in order(turn):
        send(up_s.at[dest], at_rows(up_o, f), s_up.at[dest], r_up.at[f], (dest, t))
    fetch[2].wait()
    cast(dnm, dn_s, dn_o, None)

    near = (far[2], far[1], far[0])
    for zz in near:
        arrived(xg.at[t, zz, x], s_tz.at[zz], r_tz.at[zz], (zz * 2 + x, t))
        pass_on(zz)
    for xx in (x,):
        send(xg.at[t, :, xx], xg.at[t, :, xx], s_tc.at[y, xx], r_tc.at[y, xx], at_c)
    for zz in (z,) + near:
        arrived(xg.at[t, zz, ox], s_tx.at[zz], r_tx.at[zz], at_x)
        send(xg.at[t, zz, ox], xg.at[t, zz, ox], s_ty.at[zz, ox], r_ty.at[zz, ox], at_y)
    send(xg.at[t, :, ox], xg.at[t, :, ox], s_tc.at[y, ox], r_tc.at[y, ox], at_c)
    other = oy * 2 + c
    for xx in (x, ox):
        for zz in (z,) + near:
            arrived(xg.at[other, zz, xx], s_ty.at[zz, xx], r_ty.at[zz, xx], at_y)
        send(xg.at[other, :, xx], xg.at[other, :, xx], s_tc.at[oy, xx], r_tc.at[oy, xx], at_c)
    def send_down(i, dest):
        send(dn_s.at[dest, i * fine:(i + 1) * fine], at_half(dn_o, f, i),
             s_dn.at[i, dest], r_dn.at[i, f], (dest, t))

    for i in range(2):
        for dest in order(far[2:]):
            send_down(i, dest)
    for yy in (y, oy):
        for xx in (x, ox):
            part = xg.at[yy * 2 + oc, :, xx]
            arrived(part, s_tc.at[yy, xx], r_tc.at[yy, xx], at_c)

    everyone = [zz * 2 + xx for zz in far for xx in (x, ox)] + [z * 2 + ox]
    for k in everyone:
        arrived(at_rows(up_o, k), s_up.at[k], r_up.at[k], (k, t))
    crossing = (far[0] * c + far[1] * (1 - c), far[1] * c + far[0] * (1 - c))
    for i in range(2):
        for zz in crossing:
            for xx in (x, ox):
                send_down(i, zz * 2 + xx)
    keep_up = pltpu.make_async_copy(up_o, up_h, s_out.at[0])
    keep_up.start()

    span = 2 * rows

    @pl.loop(0, nz)
    def _(zz):
        total = jnp.zeros((span, units), F32)
        for q in range(4):
            total += jnp.dot(xg[q, zz].reshape(span, cols), up_o[q * cols:(q + 1) * cols, :],
                             preferred_element_type=F32)
        act[pl.ds(pl.multiple_of(zz * span, span), span), :] = jnp.square(
            jnp.maximum(total, 0.0)).astype(BF16)

    def partial(yy, cc, i, zz):
        rows_act = act[pl.ds(pl.multiple_of(zz * span, span), span), :]
        return jnp.concatenate([
            lax.dot_general(
                rows_act, at_half(dn_o, yy * 4 + cc * 2 + xx, i)[...],
                (((1,), (1,)), ((), ())), preferred_element_type=F32)
            for xx in range(2)], axis=1)

    def have(yy, cc, i):
        for xx in range(2):
            k = yy * 4 + cc * 2 + xx

            @pl.when(k != f)
            def _():
                arrived(at_half(dn_o, k, i), s_dn.at[i, k], r_dn.at[i, k], (k, t))

    def two(h):
        return pl.ds(h * 2, 2)

    def each(h, body):
        @pl.loop(0, 2)
        def _(step):
            body(h * 2 + step)

    def to_core(yy, i):
        have(yy, oc, i)

        @pl.loop(0, nz)
        def _(zz):
            cs[yy * 2 + i, zz] = partial(yy, oc, i, zz).astype(BF16)

        send(cs.at[yy * 2 + i], cr.at[yy * 2 + i], s_c.at[yy, i], r_c.at[yy, i], at_c)

    def core_sum(yy, i, zz):
        return partial(yy, c, i, zz) + cr[yy * 2 + i, zz].astype(F32)

    def halves(total, wide_ref, sent_ref, zz):
        for xx in range(2):
            half = total[xx * rows:(xx + 1) * rows]
            wide_ref[xx, zz] = half
            sent_ref[xx, zz] = half.astype(BF16)

    hs = (low, 1 - low)
    close = z // 2
    over_y = [
        pltpu.make_async_remote_copy(
            src_ref=fb.at[oy, two(h)], dst_ref=yr.at[two(h)], send_sem=s_y.at[h],
            recv_sem=r_y.at[h], device_id=at_y, device_id_type=pl.DeviceIdType.MESH)
        for h in hs]
    sent.extend(over_y)

    def stage(i, yy):
        to_core(yy, i)
        have(yy, c, i)
        arrived(cr.at[yy * 2 + i], s_c.at[yy, i], r_c.at[yy, i], at_c)
        for h in hs:
            if i == 1:
                each(h, lambda zz: halves(core_sum(yy, 1, zz), gs.at[yy], gb.at[yy], zz))
                send(gb.at[yy, ox, two(h)], gr.at[yy, two(h)],
                     s_g.at[yy, h], r_g.at[yy, h], at_x)
            else:
                def body(zz):
                    total = core_sum(yy, 0, zz)
                    fw[yy, zz] = total
                    fb[yy, zz] = total.astype(BF16)

                each(h, body)
        if i == 0:
            @pl.when(yy == oy)
            def _():
                for copy in over_y:
                    copy.start()

    pair, same = far[2], (z + 2) % 4
    across = (pair + 2) % 4
    at_pair, at_same = (pair * 2 + x, t), (same * 2 + x, t)

    def to_pair(i, place):
        if place == 0:
            send(zb.at[i, across], zr.at[i, 0], s_z.at[i, 0], r_z.at[i, 0], at_pair)
        else:
            send(zb.at[i, pair], zr.at[i, 1], s_z.at[i, 1], r_z.at[i, 1], at_pair)

    def cross(i):
        arrived(zr.at[i, 0], s_z.at[i, 0], r_z.at[i, 0], at_pair)
        zb[i, z] = (kept[i, same] + zr[i, 0].astype(F32)).astype(BF16)
        send(zb.at[i, z], zr.at[i, 2], s_z.at[i, 2], r_z.at[i, 2], at_same)

    over_h = [
        pltpu.make_async_remote_copy(
            src_ref=hb.at[two(h)], dst_ref=hr.at[two(h)], send_sem=s_h.at[h],
            recv_sem=r_h.at[h], device_id=at_y, device_id_type=pl.DeviceIdType.MESH)
        for h in hs]
    sent.extend(over_h)

    def other_half():
        for place, h in enumerate(hs):
            arrived(gr.at[oy, two(h)], s_g.at[oy, h], r_g.at[oy, h], at_x)

            def body(zz):
                hb[zz] = (gs[oy, x, zz] + gr[oy, zz].astype(F32)).astype(BF16)

            each(h, body)
            over_h[place].start()

    stage(0, close)
    stage(1, close)
    stage(0, 1 - close)
    pl.when(oy == close)(other_half)
    stage(1, 1 - close)
    for h in hs:
        arrived(yr.at[two(h)], s_y.at[h], r_y.at[h], at_y)
        each(h, lambda zz: halves(fw[y, zz] + yr[zz].astype(F32), xs, xb, zz))
        send(xb.at[ox, two(h)], xr.at[two(h)], s_x.at[h], r_x.at[h], at_x)
    pl.when(oy != close)(other_half)
    keep_dn = pltpu.make_async_copy(dn_o, dn_h, s_out.at[1])
    keep_dn.start()
    for place, h in enumerate(hs):
        arrived(xr.at[two(h)], s_x.at[h], r_x.at[h], at_x)

        def body(zz):
            total = xs[x, zz] + xr[zz].astype(F32)
            kept[0, zz] = total

            @pl.when(zz != z)
            def _():
                zb[0, zz] = total.astype(BF16)

        each(h, body)
        to_pair(0, place)
    cross(0)
    for place, h in enumerate(hs):
        arrived(gr.at[y, two(h)], s_g.at[y, h], r_g.at[y, h], at_x)
        arrived(hr.at[two(h)], s_h.at[h], r_h.at[h], at_y)

        def body(zz):
            total = gs[y, x, zz] + gr[y, zz].astype(F32) + hr[zz].astype(F32)
            kept[1, zz] = total

            @pl.when(zz != z)
            def _():
                zb[1, zz] = total.astype(BF16)

        each(h, body)
        to_pair(1, place)
        if place == 0:
            cross(1)
    for i in range(2):
        arrived(zr.at[i, 1], s_z.at[i, 1], r_z.at[i, 1], at_pair)
        arrived(zr.at[i, 2], s_z.at[i, 2], r_z.at[i, 2], at_same)
        total = (kept[i, z] + zr[i, 1].astype(F32) + zr[i, 2].astype(F32)).astype(BF16)
        for xx in range(2):
            mix_o[:, xx * feat + i * fine:xx * feat + (i + 1) * fine] = (
                total[:, xx * fine:(xx + 1) * fine])
    for copy in sent:
        copy.wait_send()
    keep_up.wait()
    keep_dn.wait()


def on_device_fused(tokens, gain, up_master, down_master):
    rows, width = tokens.shape
    feat, ff = up_master.shape
    units = ff // SUB
    nz = SUB // 2
    cols = width // 4
    span = 2 * rows
    dma = pltpu.SemaphoreType.DMA
    vmem = pl.BlockSpec(memory_space=pltpu.VMEM)
    anywhere = pl.BlockSpec(memory_space=pl.ANY)
    shapes = [(nz,), (nz,), (nz, 2), (2, 2), (SUB,), (2, SUB), (2, 2), (2,), (2, 2), (2,), (2,), (2, nz)]
    up_s, dn_s, mixed = pl.pallas_call(
        functools.partial(fused, nz),
        out_shape=(
            jax.ShapeDtypeStruct((SUB * feat, units), BF16),
            jax.ShapeDtypeStruct((SUB * feat, units), BF16),
            jax.ShapeDtypeStruct((rows, cols), BF16),
        ),
        in_specs=[anywhere, vmem, anywhere, anywhere],
        out_specs=(anywhere, anywhere, vmem),
        scratch_shapes=[
            pltpu.VMEM((rows, width), BF16),
            pltpu.VMEM((feat, ff), F32),
            pltpu.VMEM((feat, ff), F32),
            pltpu.VMEM((SUB * feat, units), BF16),
            pltpu.VMEM((SUB * feat, units), BF16),
            dma((3,)),
            dma((2,)),
            pltpu.VMEM((4, nz, 2, rows, cols), BF16),
            pltpu.VMEM((SUB, feat, units), BF16),
            pltpu.VMEM((SUB, feat, units), BF16),
            pltpu.VMEM((SUB * rows, units), BF16),
            pltpu.VMEM((4, nz, span, feat), BF16),
            pltpu.VMEM((4, nz, span, feat), BF16),
            pltpu.VMEM((2, nz, span, feat), F32),
            pltpu.VMEM((2, nz, span, feat), BF16),
            pltpu.VMEM((nz, span, feat), BF16),
            pltpu.VMEM((2, 2, nz, rows, feat), F32),
            pltpu.VMEM((2, 2, nz, rows, feat), BF16),
            pltpu.VMEM((2, nz, rows, feat), BF16),
            pltpu.VMEM((nz, rows, feat), BF16),
            pltpu.VMEM((nz, rows, feat), BF16),
            pltpu.VMEM((2, nz, rows, feat), F32),
            pltpu.VMEM((2, nz, rows, feat), BF16),
            pltpu.VMEM((nz, rows, feat), BF16),
            pltpu.VMEM((2, nz, rows, feat), F32),
            pltpu.VMEM((2, nz, rows, feat), BF16),
            pltpu.VMEM((2, nz, rows, feat), BF16),
        ] + [dma(shape) for shape in shapes for _ in range(2)],
        compiler_params=pltpu.CompilerParams(
            collective_id=0, has_side_effects=True, vmem_limit_bytes=60 * 2**20),
    )(tokens, gain[None, :], up_master, down_master)
    return up_s[None], dn_s[None], mixed


def from_partner(block, axis, bit):
    count = lax.axis_size(axis)
    route = []
    for low in range(count):
        high = low | 1 << bit
        if high != low and high < count:
            route += [(low, high), (high, low)]
    return lax.ppermute(block, axis, route)


def on_device(tokens, gain, up_master, down_master):
    fs_count = lax.axis_size("fs")
    feat_rows = up_master.shape[0]
    units = up_master.shape[1] // SUB
    groups_count = fs_count // SUB
    member = lax.axis_index("fs") % SUB
    up_round = (gain[:, None] * up_master).astype(jnp.bfloat16)
    down_round = down_master.astype(jnp.bfloat16)

    def spread(weight):
        blocks = weight.reshape(feat_rows, SUB, units).transpose(1, 0, 2)
        return jnp.broadcast_to(blocks[None], (groups_count, SUB, feat_rows, units)).reshape(
            fs_count, feat_rows, units
        )

    up_sampled, down_sampled = (
        lax.all_to_all(spread(up_round), "fs", split_axis=0, concat_axis=1, tiled=True),
        lax.all_to_all(spread(down_round), "fs", split_axis=0, concat_axis=1, tiled=True),
    )
    levels = SUB.bit_length() - 1
    bit_list = list(range(levels))
    widened = tokens.astype(jnp.float32)
    normed = (
        widened * lax.rsqrt(jnp.mean(widened * widened, axis=1, keepdims=True) + 1e-06)
    ).astype(jnp.bfloat16)
    current = normed[None]
    for bit in bit_list:
        partner = from_partner(current, "fs", bit)
        lower = member >> bit & 1 == 0
        current = jnp.where(lower, jnp.stack([current, partner]), jnp.stack([partner, current]))
    order_now = list(reversed(bit_list))
    wanted = list(range(levels - 1, -1, -1))
    perm_axes = [
        [place for place, value in enumerate(order_now) if value == target][0] for target in wanted
    ]
    current = jnp.transpose(current, perm_axes + [levels, levels + 1, levels + 2])
    gathered = current.reshape(SUB * tokens.shape[0], tokens.shape[1])
    pre_units = jnp.dot(gathered, up_sampled[0], preferred_element_type=jnp.float32)
    act_units = jnp.square(jax.nn.relu(pre_units)).astype(jnp.bfloat16)
    partial_out = lax.dot_general(
        act_units, down_sampled[0], (((1,), (1,)), ((), ())), preferred_element_type=jnp.float32
    )
    running = partial_out.reshape((2,) * levels + (tokens.shape[0], tokens.shape[1]))
    axis_bits = list(range(levels - 1, -1, -1))
    for bit in bit_list:
        position = len([value for value in axis_bits if value > bit])
        mine = member >> bit & 1
        keep = lax.dynamic_index_in_dim(running, mine, position, keepdims=False)
        other = lax.dynamic_index_in_dim(running, 1 - mine, position, keepdims=False)
        running = keep + from_partner(other, "fs", bit)
        axis_bits = [value for value in axis_bits if value != bit]
    summed = lax.psum_scatter(running, "tp", scatter_dimension=1, tiled=True)
    return (up_sampled, down_sampled, summed.astype(jnp.bfloat16))


def solution(mesh):
    placed = (P("fs", None), P("fs"), P("fs", "tp"), P("fs", "tp"))
    one_group = mesh.shape["fs"] == SUB and mesh.shape["tp"] == 4
    return jax.shard_map(
        on_device_fused if one_group else on_device,
        mesh=mesh,
        in_specs=placed,
        out_specs=(P("fs", None, "tp"), P("fs", None, "tp"), P("fs", "tp")),
        check_vma=False,
    )
```
